32 devices in a mesh: ep: 32 (over z, y, x, core).
Axes of the slice: x: 2, y: 2, z: 4, core: 2. Of those that a mesh axis runs over, the one named last changes fastest.
Arguments:
- tokens: bfloat16 [256, 2048], P('ep'), may hold values from -6 to 6
- premix_gain: float32 [2048], replicated, may hold values from 0.1 to 1.9
- postmix_gain: float32 [2048], replicated, may hold values from 0.1 to 1.9
- prefeed_gain: float32 [2048], replicated, may hold values from 0.1 to 1.9
- postfeed_gain: float32 [2048], replicated, may hold values from 0.1 to 1.9
- query_weight: bfloat16 [2048, 1024], P('ep'), may hold values from -0.125 to 0.125
- key_weight: bfloat16 [2048, 1024], P('ep'), may hold values from -0.125 to 0.125
- value_weight: bfloat16 [2048, 1024], P('ep'), may hold values from -0.125 to 0.125
- outgate_weight: bfloat16 [2048, 1024], P('ep'), may hold values from -0.125 to 0.125
- ingate_weight: bfloat16 [2048, 8], replicated, may hold values from -0.125 to 0.125
- forget_weight: bfloat16 [2048, 8], replicated, may hold values from -0.125 to 0.125
- ingate_bias: float32 [8], replicated, may hold values from -1 to 1
- forget_bias: float32 [8], replicated, may hold values from -1 to 5
- memory_state: float32 [256, 8, 128, 128], P('ep'), may hold values from -1.25 to 1.25
- normalizer: float32 [256, 8, 128], P('ep'), may hold values from -1.75 to 1.75
- stabilizer: float32 [256, 8], P('ep'), may hold values from -2 to 2
- output_weight: bfloat16 [1024, 2048], P(None, 'ep'), may hold values from -0.1875 to 0.1875
- expert_ids: int32 [256, 6], P('ep'), may hold values from 0 to 31, all different within a row; in each aligned block of 8 rows (0 to 7, 8 to 15, ...) at most 4 rows name the same one
- route_weights: float32 [256, 6], P('ep'), may hold values from 0.2 to 0.8
- expert_gate: bfloat16 [32, 2048, 512], P('ep'), may hold values from -0.125 to 0.125
- expert_up: bfloat16 [32, 2048, 512], P('ep'), may hold values from -0.125 to 0.125
- expert_down: bfloat16 [32, 512, 2048], P('ep'), may hold values from -0.25 to 0.25
- shared_gate: bfloat16 [2048, 512], replicated, may hold values from -0.125 to 0.125
- shared_up: bfloat16 [2048, 512], replicated, may hold values from -0.125 to 0.125
- shared_down: bfloat16 [512, 2048], replicated, may hold values from -0.25 to 0.25
Outputs:
- next_tokens: bfloat16 [256, 2048], P('ep')
- next_memory: float32 [256, 8, 128, 128], P('ep')
- next_normalizer: float32 [256, 8, 128], P('ep')
- next_stabilizer: float32 [256, 8], P('ep')
The draws below stay inside these ranges and needn't reach their ends.
Inputs may be any that keep to these rules, and one draw needn't show every extreme that they name: `expert_ids`: each row names 6 different experts. Among the rows of one device no expert is named more than 4 times, and in every draw some expert is named exactly 4 times by the rows of some device.
All inputs are finite; a program needn't handle non-finite values.
Results may differ from the reference program's by a relative error of at most 0.0097.
Values may be sent and summed in bfloat16 or wider, within the bound.
A program may use at most 128 MiB of HBM per device.

```python
import math
import jax
import jax.numpy as jnp
import numpy as np
from jax import lax

D = 2048
HEADS = 8
HEAD_DIM = 128
D_MEM = 1024
FF = 512
TOP_K = 6
EXPERTS = 32
SEQ_DEV = 8
SEQS = 256
CAP = 4
N_EP = 32


def block_scale(stream_key, extent, split, smallest, top_value):
    factor_of, own = 1.0, jax.random.fold_in(stream_key, 6)
    for axis_at, shards_of in split:
        heights = jnp.exp(jax.random.uniform(jax.random.fold_in(own, axis_at), (shards_of,), jnp.float32, smallest / len(split), top_value / len(split)))
        factor_of = factor_of * jnp.repeat(heights, extent[axis_at] // shards_of).reshape([-1 if axis == axis_at else 1 for axis in range(len(extent))])
    return factor_of


def deal_out(rng, own, number, rows, number_of, top, limit, slope):
    sequence = jax.random.permutation(rng, number_of)
    crowded, usual = portions_of(number_of, rows * top, limit, slope, True), portions_of(number_of, rows * top, limit, slope, False)
    places = jnp.arange(number_of)

    def named(lengths, rotation):
        used = int((lengths > 0).sum())
        fixed = max(1, used // 4)
        shifted = fixed + (places - fixed + rotation * (used - fixed)) % max(1, number_of - fixed)
        return jnp.zeros((number_of,), jnp.int32).at[sequence[jnp.where(places < fixed, places, shifted)]].set(jnp.asarray(lengths, jnp.int32))

    lengths = jnp.where(number % 4 == 0, named(crowded, number // 4), named(usual, number - number // 4 - 1))
    mixed = jax.random.permutation(jax.random.fold_in(own, 3), number_of)
    donor, taker = mixed[0:number_of // 2 * 2:2], mixed[1:number_of // 2 * 2:2]
    margin = jnp.minimum(lengths[donor] - 1, limit - lengths[taker]) // 2
    margin = jnp.where((donor == sequence[0]) | (taker == sequence[0]) | (lengths[taker] == 0), 0, jnp.maximum(margin, 0))
    shifted = jax.random.randint(jax.random.fold_in(own, 4), (number_of // 2,), 0, 1 << 20) % (margin + 1)
    lengths = lengths.at[donor].add(-shifted).at[taker].add(shifted)
    labels = jnp.searchsorted(jnp.cumsum(lengths), jnp.arange(rows * top), side="right").astype(jnp.int32)
    listing = labels.reshape(top, rows).T
    listing = listing[jax.random.permutation(jax.random.fold_in(own, 1), rows)]
    rotation = jax.random.randint(jax.random.fold_in(own, 2), (rows, 1), 0, top)
    return jnp.take_along_axis(listing, (jnp.arange(top)[None, :] + rotation) % top, axis=1)


def portions_of(number_of, total, limit, skew, full):
    weights = [(1 << 20) // math.isqrt(rank ** skew) + 1 for rank in range(1, number_of + 1)]
    largest = limit if full else min(limit, max(-(-total // number_of), total * weights[0] // sum(weights)))
    least = 1 if total - largest >= number_of - 1 else 0
    given, rest = [largest] + [least] * (number_of - 1), total - largest - least * (number_of - 1)
    while rest > 0:
        free = [i for i in range(1, number_of) if given[i] < largest] or [i for i in range(1, number_of) if given[i] < limit]
        pool, left = sum([weights[i] for i in free]), rest
        for i in free:
            addition = min(limit - given[i], max(1, left * weights[i] // pool), rest)
            given[i] = given[i] + addition
            rest = rest - addition
    return np.array(given)


def noise(own_key, extent, scale, bound, shards=(), kind=jnp.bfloat16):
    result = scale * jax.random.normal(own_key, extent, jnp.float32)
    if shards:
        result = result * block_scale(own_key, extent, shards, -0.22, 0.18)
    return jnp.clip(result, -bound, bound).astype(kind)


def setup_inputs(seed: int = 0) -> dict:
    streams_of = jax.random.split(jax.random.key(seed), 26)
    tokens = noise(streams_of[0], (SEQS, D), 1.0, 6.0, ((0, 32),))
    premix_gain = jnp.clip(1.0 + 0.18 * jax.random.normal(streams_of[1], (D,), jnp.float32), 0.1, 1.9)
    postmix_gain = jnp.clip(1.0 + 0.18 * jax.random.normal(streams_of[2], (D,), jnp.float32), 0.1, 1.9)
    prefeed_gain = jnp.clip(1.0 + 0.18 * jax.random.normal(streams_of[3], (D,), jnp.float32), 0.1, 1.9)
    postfeed_gain = jnp.clip(1.0 + 0.18 * jax.random.normal(streams_of[4], (D,), jnp.float32), 0.1, 1.9)
    query_weight = noise(streams_of[5], (D, D_MEM), D ** -0.5, 0.125, ((0, 32),))
    key_weight = noise(streams_of[6], (D, D_MEM), D ** -0.5, 0.125, ((0, 32),))
    value_weight = noise(streams_of[7], (D, D_MEM), D ** -0.5, 0.125, ((0, 32),))
    outgate_weight = noise(streams_of[8], (D, D_MEM), D ** -0.5, 0.125, ((0, 32),))
    ingate_weight = noise(streams_of[9], (D, HEADS), D ** -0.5, 0.125)
    forget_weight = noise(streams_of[10], (D, HEADS), D ** -0.5, 0.125)
    ingate_bias = jnp.clip(jax.random.uniform(streams_of[11], (HEADS,), jnp.float32, -1.0, 1.0), -1.0, 1.0)
    forget_bias = jnp.clip(jax.random.uniform(streams_of[12], (HEADS,), jnp.float32, -1.0, 5.0), -1.0, 5.0)
    memory_state = noise(streams_of[13], (SEQS, HEADS, HEAD_DIM, HEAD_DIM), 0.2, 1.25, ((0, 32),), jnp.float32)
    normalizer = noise(streams_of[14], (SEQS, HEADS, HEAD_DIM), 0.3, 1.75, ((0, 32),), jnp.float32)
    stabilizer = jnp.clip(jax.random.uniform(streams_of[15], (SEQS, HEADS), jnp.float32, -2.0, 2.0) * block_scale(streams_of[15], (SEQS, HEADS), ((0, 32),), -0.4, 0.0), -2.0, 2.0)
    output_weight = noise(streams_of[16], (D_MEM, D), D_MEM ** -0.5, 0.1875, ((1, 32),))
    expert_ids_keys = jax.random.split(jax.random.fold_in(streams_of[17], 1), SEQS // SEQ_DEV)
    expert_ids_turns = jax.random.permutation(jax.random.fold_in(streams_of[17], 3), SEQS // SEQ_DEV)
    expert_ids = jax.vmap(lambda own, number: deal_out(jax.random.fold_in(streams_of[17], 2), own, number, SEQ_DEV, EXPERTS, TOP_K, CAP, 2))(expert_ids_keys, expert_ids_turns).reshape((SEQS, TOP_K))
    route_weights = jnp.clip(0.2 + 0.6 * jax.random.uniform(streams_of[18], (SEQS, TOP_K), jnp.float32) ** block_scale(streams_of[18], (SEQS, TOP_K), ((0, 32),), -0.2, 0.2), 0.2, 0.8)
    expert_gate = noise(streams_of[19], (EXPERTS, D, FF), D ** -0.5, 0.125, ((0, 32),))
    expert_up = noise(streams_of[20], (EXPERTS, D, FF), D ** -0.5, 0.125, ((0, 32),))
    expert_down = noise(streams_of[21], (EXPERTS, FF, D), FF ** -0.5, 0.25, ((0, 32),))
    shared_gate = noise(streams_of[22], (D, FF), D ** -0.5, 0.125)
    shared_up = noise(streams_of[23], (D, FF), D ** -0.5, 0.125)
    shared_down = noise(streams_of[24], (FF, D), FF ** -0.5, 0.25)
    return dict(tokens=tokens, premix_gain=premix_gain, postmix_gain=postmix_gain, prefeed_gain=prefeed_gain, postfeed_gain=postfeed_gain, query_weight=query_weight, key_weight=key_weight, value_weight=value_weight, outgate_weight=outgate_weight, ingate_weight=ingate_weight, forget_weight=forget_weight, ingate_bias=ingate_bias, forget_bias=forget_bias, memory_state=memory_state, normalizer=normalizer, stabilizer=stabilizer, output_weight=output_weight, expert_ids=expert_ids, route_weights=route_weights, expert_gate=expert_gate, expert_up=expert_up, expert_down=expert_down, shared_gate=shared_gate, shared_up=shared_up, shared_down=shared_down)


epsilon = 1e-06

def rms_scale(values, gain_row):
    return values * lax.rsqrt(lax.optimization_barrier(jnp.mean(values * values, axis=-1, keepdims=True)) + epsilon) * gain_row

def rounded(values):
    return lax.optimization_barrier(values.astype(jnp.bfloat16))

def memory_step(queries, key_rows, value_rows, out_gate, input_pre, forget_pre, memory_state, normalizer, stabilizer):
    sequences = queries.shape[0]
    head_count = memory_state.shape[1]
    head_width = memory_state.shape[2]
    query_heads = queries.astype(jnp.float32).reshape(sequences, head_count, head_width)
    key_heads = key_rows.astype(jnp.float32).reshape(sequences, head_count, head_width) * head_width ** (-0.5)
    value_heads = value_rows.astype(jnp.float32).reshape(sequences, head_count, head_width)
    carried = jax.nn.log_sigmoid(forget_pre) + stabilizer
    next_stabilizer = jnp.maximum(carried, input_pre)
    keep_old = jnp.exp(carried - next_stabilizer)
    write_new = jnp.exp(input_pre - next_stabilizer)
    local_score = write_new * lax.optimization_barrier(jnp.sum(query_heads * key_heads, axis=-1))
    read_memory = jnp.einsum('shvk,shk->shv', memory_state, query_heads, precision=lax.Precision.HIGHEST)
    numerator = keep_old[..., None] * read_memory + local_score[..., None] * value_heads
    denominator = keep_old * lax.optimization_barrier(jnp.sum(normalizer * query_heads, axis=-1)) + local_score
    memory_read = numerator / jnp.maximum(jnp.abs(denominator), 1.0)[..., None]
    gated_out = (jax.nn.sigmoid(out_gate.astype(jnp.float32)) * memory_read.reshape(sequences, head_count * head_width)).astype(jnp.bfloat16)
    next_memory = keep_old[..., None, None] * memory_state + write_new[..., None, None] * value_heads[..., :, None] * key_heads[..., None, :]
    next_normalizer = keep_old[..., None] * normalizer + write_new[..., None] * key_heads
    return (gated_out, next_memory, next_normalizer, next_stabilizer)

def expert_rows(row_block, gate_weight, up_weight, down_weight):
    gate_values = jnp.dot(row_block, gate_weight, preferred_element_type=jnp.float32)
    up_values = jnp.dot(row_block, up_weight, preferred_element_type=jnp.float32)
    inner_rows = (jax.nn.silu(gate_values) * up_values).astype(jnp.bfloat16)
    return jnp.dot(inner_rows, down_weight, preferred_element_type=jnp.float32)

def reference(tokens, premix_gain, postmix_gain, prefeed_gain, postfeed_gain, query_weight, key_weight, value_weight, outgate_weight, ingate_weight, forget_weight, ingate_bias, forget_bias, memory_state, normalizer, stabilizer, output_weight, expert_ids, route_weights, expert_gate, expert_up, expert_down, shared_gate, shared_up, shared_down):
    residual = tokens.astype(jnp.float32)
    normed = rms_scale(residual, premix_gain).astype(jnp.bfloat16)
    queries = rounded(jnp.dot(normed, query_weight, preferred_element_type=jnp.float32))
    key_rows = rounded(jnp.dot(normed, key_weight, preferred_element_type=jnp.float32))
    value_rows = rounded(jnp.dot(normed, value_weight, preferred_element_type=jnp.float32))
    out_gate = rounded(jnp.dot(normed, outgate_weight, preferred_element_type=jnp.float32))
    input_pre = jnp.dot(normed, ingate_weight, preferred_element_type=jnp.float32) + ingate_bias
    forget_pre = jnp.dot(normed, forget_weight, preferred_element_type=jnp.float32) + forget_bias
    gated_out, next_memory, next_normalizer, next_stabilizer = memory_step(queries, key_rows, value_rows, out_gate, input_pre, forget_pre, memory_state, normalizer, stabilizer)
    mixed = rounded(jnp.dot(gated_out, output_weight, preferred_element_type=jnp.float32))
    after_mix = rounded(residual + rms_scale(mixed.astype(jnp.float32), postmix_gain))
    after_float = after_mix.astype(jnp.float32)
    expert_input = rms_scale(after_float, prefeed_gain).astype(jnp.bfloat16)
    flat_ids = expert_ids.reshape(-1).astype(jnp.int32)
    one_hot = (flat_ids[:, None] == jnp.arange(EXPERTS, dtype=jnp.int32)[None, :]).astype(jnp.int32)
    earlier = jnp.cumsum(one_hot, axis=0) - one_hot
    slot_ids = lax.optimization_barrier(jnp.sum(earlier * one_hot, axis=1)).astype(jnp.int32)
    token_index = (jnp.arange(SEQS * TOP_K, dtype=jnp.int32) // TOP_K).astype(jnp.int32)
    slot_table = jnp.zeros((EXPERTS, N_EP * CAP), jnp.int32).at[flat_ids, slot_ids].set(token_index)

    def one_expert(inputs):
        rows_index, gate_weight, up_weight, down_weight = inputs
        return expert_rows(expert_input[rows_index], gate_weight, up_weight, down_weight).astype(jnp.bfloat16)
    outputs = lax.map(one_expert, (slot_table, expert_gate, expert_up, expert_down))
    picked = outputs[flat_ids, slot_ids].astype(jnp.float32).reshape(SEQS, TOP_K, D)
    routed = lax.optimization_barrier(jnp.sum(picked * route_weights[:, :, None], axis=1))
    shared_out = expert_rows(expert_input, shared_gate, shared_up, shared_down)
    next_tokens = (after_float + rms_scale(routed + shared_out, postfeed_gain)).astype(jnp.bfloat16)
    return (next_tokens, next_memory, next_normalizer, next_stabilizer)
```

```python
import functools

import jax
import jax.numpy as jnp
from jax import lax
from jax.experimental import pallas as pl
from jax.experimental.pallas import tpu as pltpu
from jax.sharding import PartitionSpec as P

epsilon = 1e-06
LANES = 128
MESH = pl.DeviceIdType.MESH
VM = pl.BlockSpec(memory_space=pltpu.VMEM)
ANY = pl.BlockSpec(memory_space=pl.ANY)


def rms_scale(values, gain_row):
    return (
        values * lax.rsqrt(jnp.mean(values * values, axis=-1, keepdims=True) + epsilon) * gain_row
    )


def rounded(values):
    return lax.optimization_barrier(values.astype(jnp.bfloat16))


def greet(n, me):
    sem = pltpu.get_barrier_semaphore()

    def signal(i, carry):
        pl.semaphore_signal(
            sem, inc=1, device_id=(lax.rem(me + i, n),), device_id_type=MESH
        )
        return carry

    lax.fori_loop(1, n, signal, 0)


def greeted(n):
    pl.semaphore_wait(pltpu.get_barrier_semaphore(), n - 1)


def send(src, dst, send_sem, recv_sem, peer):
    pltpu.make_async_remote_copy(
        src_ref=src,
        dst_ref=dst,
        send_sem=send_sem,
        recv_sem=recv_sem,
        device_id=(peer,),
        device_id_type=MESH,
    ).start()


def drain(ref, sem):
    pltpu.make_async_copy(ref, ref, sem).wait()


def project_kernel(
    n,
    groups,
    normed_ref,
    query_ref,
    key_ref,
    value_ref,
    gate_ref,
    out_ref,
    rows_buf,
    weight_buf,
    product_buf,
    result_buf,
    send_sems,
    recv_sems,
):
    me = lax.axis_index("ep")
    blocks = n // groups
    per_matrix = blocks // 4
    mine, turn = me // groups, lax.rem(me, groups)
    greet(n, me)
    weights = (query_ref, key_ref, value_ref, gate_ref)

    def column(block):
        return pl.ds(pl.multiple_of(lax.rem(block, per_matrix) * LANES, LANES), LANES)

    for index, ref in enumerate(weights):

        @pl.when(mine // per_matrix == index)
        def _():
            pltpu.make_async_copy(
                ref.at[:, column(mine)], weight_buf.at[me], recv_sems.at[1]
            ).start()

    pltpu.make_async_copy(normed_ref, rows_buf.at[mine], recv_sems.at[0]).start()
    greeted(n)

    def send_rows(i, carry):
        place = lax.rem(mine + i, blocks)
        send(
            normed_ref,
            rows_buf.at[mine],
            send_sems.at[0],
            recv_sems.at[0],
            place * groups + turn,
        )
        return carry

    def send_weights(i, carry):
        peer = lax.rem(me + i, n)
        block = peer // groups
        for index, ref in enumerate(weights):

            @pl.when(block // per_matrix == index)
            def _():
                send(
                    ref.at[:, column(block)],
                    weight_buf.at[me],
                    send_sems.at[1],
                    recv_sems.at[1],
                    peer,
                )

        return carry

    lax.fori_loop(1, n, send_weights, 0)
    lax.fori_loop(1, blocks, send_rows, 0)
    drain(rows_buf, recv_sems.at[0])
    drain(weight_buf, recv_sems.at[1])
    rows = rows_buf[...].reshape(rows_buf.shape[0] * rows_buf.shape[1], rows_buf.shape[2])
    weight = weight_buf[...].reshape(weight_buf.shape[0] * weight_buf.shape[1], LANES)
    product = jnp.dot(rows, weight, preferred_element_type=jnp.float32)
    product_buf[...] = product.reshape(product_buf.shape).astype(jnp.bfloat16)
    pltpu.make_async_copy(product_buf.at[mine], result_buf.at[mine], recv_sems.at[2]).start()

    def send_product(i, carry):
        place = lax.rem(mine + i, blocks)
        send(
            product_buf.at[place],
            result_buf.at[mine],
            send_sems.at[2],
            recv_sems.at[2],
            place * groups + turn,
        )
        return carry

    lax.fori_loop(1, blocks, send_product, 0)
    drain(result_buf, recv_sems.at[2])
    for block in range(blocks):
        out_ref[:, block * LANES : (block + 1) * LANES] = result_buf[block].astype(jnp.float32)
    drain(rows_buf.at[pl.ds(0, blocks - 1)], send_sems.at[0])
    drain(weight_buf.at[pl.ds(0, n - 1)], send_sems.at[1])
    drain(result_buf.at[pl.ds(0, blocks - 1)], send_sems.at[2])


def project(n, normed, *weights):
    sequences, width = normed.shape
    depth, columns = weights[0].shape
    blocks = 4 * columns // LANES
    groups = n // blocks
    return pl.pallas_call(
        functools.partial(project_kernel, n, groups),
        out_shape=jax.ShapeDtypeStruct((sequences, 4 * columns), jnp.float32),
        in_specs=[VM, ANY, ANY, ANY, ANY],
        out_specs=VM,
        scratch_shapes=[
            pltpu.VMEM((blocks, sequences, width), jnp.bfloat16),
            pltpu.VMEM((n, depth, LANES), jnp.bfloat16),
            pltpu.VMEM((blocks, sequences, LANES), jnp.bfloat16),
            pltpu.VMEM((blocks, sequences, LANES), jnp.bfloat16),
            pltpu.SemaphoreType.DMA((3,)),
            pltpu.SemaphoreType.DMA((3,)),
        ],
        compiler_params=pltpu.CompilerParams(collective_id=0, has_side_effects=True),
    )(normed, *weights)


def mix_kernel(
    n, gated_ref, weight_ref, out_ref, rows_buf, product_buf, result_buf, send_sems, recv_sems
):
    me = lax.axis_index("ep")
    greet(n, me)
    pltpu.make_async_copy(gated_ref, rows_buf.at[me], recv_sems.at[0]).start()
    greeted(n)

    def send_rows(i, carry):
        send(
            gated_ref, rows_buf.at[me], send_sems.at[0], recv_sems.at[0], lax.rem(me + i, n)
        )
        return carry

    lax.fori_loop(1, n, send_rows, 0)
    drain(rows_buf, recv_sems.at[0])
    rows = rows_buf[...].reshape(rows_buf.shape[0] * rows_buf.shape[1], rows_buf.shape[2])
    product = jnp.dot(rows, weight_ref[...], preferred_element_type=jnp.float32)
    product_buf[...] = product.reshape(product_buf.shape).astype(jnp.bfloat16)
    pltpu.make_async_copy(product_buf.at[me], result_buf.at[me], recv_sems.at[1]).start()

    def send_product(i, carry):
        peer = lax.rem(me + i, n)
        send(product_buf.at[peer], result_buf.at[me], send_sems.at[1], recv_sems.at[1], peer)
        return carry

    lax.fori_loop(1, n, send_product, 0)
    drain(result_buf, recv_sems.at[1])
    out_ref[...] = result_buf[...]
    drain(rows_buf.at[pl.ds(0, n - 1)], send_sems.at[0])
    drain(result_buf.at[pl.ds(0, n - 1)], send_sems.at[1])


def mix(n, gated, weight):
    sequences, width = gated.shape
    columns = weight.shape[1]
    return pl.pallas_call(
        functools.partial(mix_kernel, n),
        out_shape=jax.ShapeDtypeStruct((n, sequences, columns), jnp.bfloat16),
        in_specs=[VM, VM],
        out_specs=VM,
        scratch_shapes=[
            pltpu.VMEM((n, sequences, width), jnp.bfloat16),
            pltpu.VMEM((n, sequences, columns), jnp.bfloat16),
            pltpu.VMEM((n, sequences, columns), jnp.bfloat16),
            pltpu.SemaphoreType.DMA((2,)),
            pltpu.SemaphoreType.DMA((2,)),
        ],
        compiler_params=pltpu.CompilerParams(collective_id=1, has_side_effects=True),
    )(gated, weight)


def two_layer(rows, gate_weight, up_weight, down_weight):
    gate_values = jnp.dot(rows, gate_weight, preferred_element_type=jnp.float32)
    up_values = jnp.dot(rows, up_weight, preferred_element_type=jnp.float32)
    inner_rows = (gate_values * jax.nn.sigmoid(gate_values) * up_values).astype(jnp.bfloat16)
    return jnp.dot(inner_rows, down_weight, preferred_element_type=jnp.float32)


def expert_kernel(
    n,
    rows_ref,
    dispatch_ref,
    combine_ref,
    *refs,
):
    weights_hbm, out_ref = refs[:6], refs[6]
    weights, (outgoing, arrived, answer, returned, load_sems, send_sems, recv_sems) = (
        refs[7:13],
        refs[13:],
    )
    me = lax.axis_index("ep")
    greet(n, me)
    loads = [
        pltpu.make_async_copy(source, target, load_sems.at[index])
        for index, (source, target) in enumerate(zip(weights_hbm, weights))
    ]
    for index in (3, 4, 5, 0, 1, 2):
        loads[index].start()
    local, capacity = weights[0].shape[0], outgoing.shape[2]
    width = rows_ref.shape[1]
    outgoing[...] = jnp.dot(
        dispatch_ref[...], rows_ref[...], preferred_element_type=jnp.float32
    ).reshape(outgoing.shape).astype(jnp.bfloat16)
    pltpu.make_async_copy(outgoing.at[me], arrived.at[me], recv_sems.at[0]).start()
    greeted(n)

    def exchange(source, target, stage):
        def one(i, carry):
            peer = lax.rem(me + i, n)
            send(source.at[peer], target.at[me], send_sems.at[stage], recv_sems.at[stage], peer)
            return carry

        lax.fori_loop(1, n, one, 0)

    exchange(outgoing, arrived, 0)
    for index in (3, 4, 5):
        loads[index].wait()
    shared_out = two_layer(
        rows_ref[...], weights[3][...], weights[4][...], weights[5][...]
    )
    for index in (0, 1, 2):
        loads[index].wait()
    drain(arrived, recv_sems.at[0])
    for item in range(local):
        block = arrived[:, item].astype(jnp.float32).reshape(n * capacity, width)
        answer[:, item] = (
            two_layer(
                block.astype(jnp.bfloat16),
                weights[0][item],
                weights[1][item],
                weights[2][item],
            )
            .reshape(n, capacity, width)
            .astype(jnp.bfloat16)
        )
    pltpu.make_async_copy(answer.at[me], returned.at[me], recv_sems.at[1]).start()
    exchange(answer, returned, 1)
    combine = combine_ref[...]
    high = combine.astype(jnp.bfloat16)
    low = (combine - high.astype(jnp.float32)).astype(jnp.bfloat16)
    drain(returned, recv_sems.at[1])
    picked = (
        returned[...].astype(jnp.float32).reshape(combine.shape[1], width).astype(jnp.bfloat16)
    )
    out_ref[...] = (
        shared_out
        + jnp.dot(high, picked, preferred_element_type=jnp.float32)
        + jnp.dot(low, picked, preferred_element_type=jnp.float32)
    )
    drain(arrived.at[pl.ds(0, n - 1)], send_sems.at[0])
    drain(returned.at[pl.ds(0, n - 1)], send_sems.at[1])


def experts(n, rows, dispatch, combine, *weights):
    sequences, width = rows.shape
    local = weights[0].shape[0]
    capacity = dispatch.shape[0] // (n * local)
    slots = pltpu.VMEM((n, local, capacity, width), jnp.bfloat16)
    return pl.pallas_call(
        functools.partial(expert_kernel, n),
        out_shape=jax.ShapeDtypeStruct((sequences, width), jnp.float32),
        in_specs=[VM, VM, VM] + [ANY] * 6,
        out_specs=VM,
        scratch_shapes=[pltpu.VMEM(w.shape, w.dtype) for w in weights]
        + [slots] * 4
        + [
            pltpu.SemaphoreType.DMA((6,)),
            pltpu.SemaphoreType.DMA((2,)),
            pltpu.SemaphoreType.DMA((2,)),
        ],
        compiler_params=pltpu.CompilerParams(
            collective_id=2, has_side_effects=True, vmem_limit_bytes=50 * 1024 * 1024
        ),
    )(rows, dispatch, combine, *weights)


def memory_step(
    queries,
    key_rows,
    value_rows,
    out_gate,
    input_pre,
    forget_pre,
    memory_state,
    normalizer,
    stabilizer,
):
    sequences = queries.shape[0]
    head_count = memory_state.shape[1]
    head_width = memory_state.shape[2]
    query_heads = queries.astype(jnp.float32).reshape(sequences, head_count, head_width)
    key_heads = key_rows.astype(jnp.float32).reshape(
        sequences, head_count, head_width
    ) * head_width ** (-0.5)
    value_heads = value_rows.astype(jnp.float32).reshape(sequences, head_count, head_width)
    carried = jax.nn.log_sigmoid(forget_pre) + stabilizer
    next_stabilizer = jnp.maximum(carried, input_pre)
    keep_old = jnp.exp(carried - next_stabilizer)
    write_new = jnp.exp(input_pre - next_stabilizer)
    local_score = write_new * jnp.sum(query_heads * key_heads, axis=-1)
    read_memory = jnp.einsum(
        "shvk,shk->shv", memory_state, query_heads, precision=lax.Precision.HIGHEST
    )
    numerator = keep_old[..., None] * read_memory + local_score[..., None] * value_heads
    denominator = keep_old * jnp.sum(normalizer * query_heads, axis=-1) + local_score
    memory_read = numerator / jnp.maximum(jnp.abs(denominator), 1.0)[..., None]
    gated_out = (
        jax.nn.sigmoid(out_gate.astype(jnp.float32))
        * memory_read.reshape(sequences, head_count * head_width)
    ).astype(jnp.bfloat16)
    next_memory = (
        keep_old[..., None, None] * memory_state
        + write_new[..., None, None] * value_heads[..., :, None] * key_heads[..., None, :]
    )
    next_normalizer = keep_old[..., None] * normalizer + write_new[..., None] * key_heads
    return (gated_out, next_memory, next_normalizer, next_stabilizer)


def on_device(
    tokens,
    premix_gain,
    postmix_gain,
    prefeed_gain,
    postfeed_gain,
    query_weight,
    key_weight,
    value_weight,
    outgate_weight,
    ingate_weight,
    forget_weight,
    ingate_bias,
    forget_bias,
    memory_state,
    normalizer,
    stabilizer,
    output_weight,
    expert_ids,
    route_weights,
    expert_gate,
    expert_up,
    expert_down,
    shared_gate,
    shared_up,
    shared_down,
):
    sequences = tokens.shape[0]
    model_width = tokens.shape[1]
    memory_width = query_weight.shape[1]
    devices = lax.axis_size("ep")
    residual = tokens.astype(jnp.float32)
    normed = rms_scale(residual, premix_gain).astype(jnp.bfloat16)
    projected = project(devices, normed, query_weight, key_weight, value_weight, outgate_weight)
    projected = projected.reshape(sequences, 4, memory_width)
    input_pre = jnp.dot(normed, ingate_weight, preferred_element_type=jnp.float32) + ingate_bias
    forget_pre = jnp.dot(normed, forget_weight, preferred_element_type=jnp.float32) + forget_bias
    gated_out, next_memory, next_normalizer, next_stabilizer = memory_step(
        projected[:, 0],
        projected[:, 1],
        projected[:, 2],
        projected[:, 3],
        input_pre,
        forget_pre,
        memory_state,
        normalizer,
        stabilizer,
    )
    mixed_cols = mix(devices, gated_out, output_weight)
    mixed = jnp.swapaxes(mixed_cols, 0, 1).reshape(sequences, model_width)
    after_mix = rounded(residual + rms_scale(mixed.astype(jnp.float32), postmix_gain))
    after_float = after_mix.astype(jnp.float32)
    expert_input = rms_scale(after_float, prefeed_gain).astype(jnp.bfloat16)
    local_count = expert_gate.shape[0]
    experts_total = local_count * devices
    choose_count = expert_ids.shape[1]
    capacity = min(
        sequences, max(2, 2 * ((sequences * choose_count + experts_total - 1) // experts_total))
    )
    named = (expert_ids[:, :, None] == jnp.arange(experts_total, dtype=jnp.int32)).astype(
        jnp.float32
    )
    chosen = jnp.sum(named, axis=1)
    weight_of = jnp.sum(named * route_weights[:, :, None], axis=1)
    order = jnp.arange(sequences)
    before = (order[:, None] > order[None, :]).astype(jnp.float32)
    earlier = jnp.sum(before[:, :, None] * chosen[None, :, :], axis=1)
    slots = jnp.where(
        earlier[:, :, None] == jnp.arange(capacity, dtype=jnp.float32), chosen[:, :, None], 0.0
    )
    combine = (slots * weight_of[:, :, None]).reshape(sequences, experts_total * capacity)
    dispatch = slots.reshape(sequences, experts_total * capacity).T.astype(jnp.bfloat16)
    combined = experts(
        devices,
        expert_input,
        dispatch,
        combine,
        expert_gate,
        expert_up,
        expert_down,
        shared_gate,
        shared_up,
        shared_down,
    )
    next_tokens = (after_float + rms_scale(combined, postfeed_gain)).astype(jnp.bfloat16)
    return (next_tokens, next_memory, next_normalizer, next_stabilizer)


def solution(mesh):
    in_specs = (
        P("ep", None),
        P(),
        P(),
        P(),
        P(),
        P("ep", None),
        P("ep", None),
        P("ep", None),
        P("ep", None),
        P(),
        P(),
        P(),
        P(),
        P("ep", None, None, None),
        P("ep", None, None),
        P("ep", None),
        P(None, "ep"),
        P("ep", None),
        P("ep", None),
        P("ep", None, None),
        P("ep", None, None),
        P("ep", None, None),
        P(),
        P(),
        P(),
    )
    out_specs = (P("ep", None), P("ep", None, None, None), P("ep", None, None), P("ep", None))
    return jax.shard_map(
        on_device, mesh=mesh, in_specs=in_specs, out_specs=out_specs, check_vma=False
    )
```

```python
import functools

import jax
import jax.numpy as jnp
from jax import lax
from jax.experimental import pallas as pl
from jax.experimental.pallas import tpu as pltpu
from jax.sharding import PartitionSpec as P

epsilon = 1e-06
LANES = 128
GROUPS = 4
MESH = pl.DeviceIdType.MESH
VM = pl.BlockSpec(memory_space=pltpu.VMEM)
ANY = pl.BlockSpec(memory_space=pl.ANY)


def rms_scale(values, gain_row):
    return (
        values * lax.rsqrt(jnp.mean(values * values, axis=-1, keepdims=True) + epsilon) * gain_row
    )


def rounded(values):
    return lax.optimization_barrier(values.astype(jnp.bfloat16))


def greet(n, me):
    sem = pltpu.get_barrier_semaphore()

    def signal(i, carry):
        pl.semaphore_signal(
            sem, inc=1, device_id=(lax.rem(me + i, n),), device_id_type=MESH
        )
        return carry

    lax.fori_loop(1, n, signal, 0)


def greeted(n):
    pl.semaphore_wait(pltpu.get_barrier_semaphore(), n - 1)


def send(src, dst, send_sem, recv_sem, peer):
    pltpu.make_async_remote_copy(
        src_ref=src,
        dst_ref=dst,
        send_sem=send_sem,
        recv_sem=recv_sem,
        device_id=(peer,),
        device_id_type=MESH,
    ).start()


def drain(ref, sem):
    pltpu.make_async_copy(ref, ref, sem).wait()


def project_kernel(
    n,
    groups,
    normed_ref,
    query_ref,
    key_ref,
    value_ref,
    gate_ref,
    mix_ref,
    out_ref,
    mix_all_ref,
    rows_buf,
    weight_buf,
    product_buf,
    result_buf,
    send_sems,
    recv_sems,
):
    me = lax.axis_index("ep")
    members = n // groups
    plane, place = me // members, lax.rem(me, members)
    width = rows_buf.shape[2]
    columns = weight_buf.shape[2]
    per_matrix = query_ref.shape[1] // columns
    greet(n, me)
    weights = (query_ref, key_ref, value_ref, gate_ref)

    def column(block):
        return pl.ds(pl.multiple_of(lax.rem(block, per_matrix) * columns, LANES), columns)

    def part(index):
        return normed_ref.at[:, pl.ds(pl.multiple_of(index * width, LANES), width)]

    for index, ref in enumerate(weights):

        @pl.when(place // per_matrix == index)
        def _():
            pltpu.make_async_copy(
                ref.at[:, column(place)], weight_buf.at[place], recv_sems.at[1]
            ).start()

    pltpu.make_async_copy(part(plane), rows_buf.at[me], recv_sems.at[0]).start()
    pltpu.make_async_copy(mix_ref, mix_all_ref.at[place], recv_sems.at[3]).start()
    greeted(n)

    def send_rows(i, carry):
        peer = lax.rem(me + i, n)
        send(
            part(peer // members), rows_buf.at[me], send_sems.at[0], recv_sems.at[0], peer
        )
        return carry

    def send_weights(i, carry):
        block = lax.rem(place + i, members)
        for index, ref in enumerate(weights):

            @pl.when(block // per_matrix == index)
            def _():
                send(
                    ref.at[:, column(block)],
                    weight_buf.at[place],
                    send_sems.at[1],
                    recv_sems.at[1],
                    plane * members + block,
                )

        return carry

    lax.fori_loop(1, members, send_weights, 0)
    lax.fori_loop(1, n, send_rows, 0)
    drain(rows_buf, recv_sems.at[0])
    drain(weight_buf, recv_sems.at[1])
    rows = rows_buf[...].reshape(rows_buf.shape[0] * rows_buf.shape[1], width)
    weight = weight_buf[...].reshape(weight_buf.shape[0] * weight_buf.shape[1], columns)
    product = jnp.dot(rows, weight, preferred_element_type=jnp.float32)
    product_buf[...] = product.reshape(product_buf.shape).astype(jnp.bfloat16)
    pltpu.make_async_copy(product_buf.at[me], result_buf.at[me], recv_sems.at[2]).start()

    def send_product(i, carry):
        peer = lax.rem(me + i, n)
        send(product_buf.at[peer], result_buf.at[me], send_sems.at[2], recv_sems.at[2], peer)
        return carry

    def send_mix(i, carry):
        send(
            mix_ref,
            mix_all_ref.at[place],
            send_sems.at[3],
            recv_sems.at[3],
            plane * members + lax.rem(place + i, members),
        )
        return carry

    lax.fori_loop(1, n, send_product, 0)
    lax.fori_loop(1, members, send_mix, 0)
    drain(result_buf, recv_sems.at[2])
    for member in range(members):
        total = result_buf[member].astype(jnp.float32)
        for group in range(1, groups):
            total = total + result_buf[group * members + member].astype(jnp.float32)
        out_ref[:, member * columns : (member + 1) * columns] = total
    drain(mix_all_ref, recv_sems.at[3])
    drain(rows_buf.at[pl.ds(0, n - 1)], send_sems.at[0])
    drain(weight_buf.at[pl.ds(0, members - 1)], send_sems.at[1])
    drain(result_buf.at[pl.ds(0, n - 1)], send_sems.at[2])
    drain(mix_all_ref.at[pl.ds(0, members - 1)], send_sems.at[3])


def project(n, groups, normed, mix_weight, *weights):
    sequences, width = normed.shape
    depth, columns = weights[0].shape
    members = n // groups
    wide = 4 * columns // members
    return pl.pallas_call(
        functools.partial(project_kernel, n, groups),
        out_shape=(
            jax.ShapeDtypeStruct((sequences, 4 * columns), jnp.float32),
            jax.ShapeDtypeStruct((members,) + mix_weight.shape, jnp.bfloat16),
        ),
        in_specs=[VM, ANY, ANY, ANY, ANY, VM],
        out_specs=(VM, ANY),
        scratch_shapes=[
            pltpu.VMEM((n, sequences, width // groups), jnp.bfloat16),
            pltpu.VMEM((members, depth, wide), jnp.bfloat16),
            pltpu.VMEM((n, sequences, wide), jnp.bfloat16),
            pltpu.VMEM((n, sequences, wide), jnp.bfloat16),
            pltpu.SemaphoreType.DMA((4,)),
            pltpu.SemaphoreType.DMA((4,)),
        ],
        compiler_params=pltpu.CompilerParams(collective_id=0, has_side_effects=True),
    )(normed, *weights, mix_weight)


def two_layer(rows, gate_weight, up_weight, down_weight):
    gate_values = jnp.dot(rows, gate_weight, preferred_element_type=jnp.float32)
    up_values = jnp.dot(rows, up_weight, preferred_element_type=jnp.float32)
    inner_rows = (gate_values * jax.nn.sigmoid(gate_values) * up_values).astype(jnp.bfloat16)
    return jnp.dot(inner_rows, down_weight, preferred_element_type=jnp.float32)


def tail_kernel(
    n,
    groups,
    gated_ref,
    tokens_ref,
    postmix_ref,
    prefeed_ref,
    postfeed_ref,
    dispatch_ref,
    combine_ref,
    *refs,
):
    weights_hbm, out_ref = refs[:7], refs[7]
    weights, (
        gated_buf,
        product_buf,
        mixed_buf,
        outgoing,
        arrived,
        answer,
        returned,
        load_sems,
        send_sems,
        recv_sems,
    ) = (
        refs[8:15],
        refs[15:],
    )
    me = lax.axis_index("ep")
    members = n // groups
    plane, place = me // members, lax.rem(me, members)
    greet(n, me)
    loads = [
        pltpu.make_async_copy(source, target, load_sems.at[index])
        for index, (source, target) in enumerate(zip(weights_hbm, weights))
    ]
    for index in (6, 3, 4, 5, 0, 1, 2):
        loads[index].start()
    pltpu.make_async_copy(gated_ref, gated_buf.at[plane], recv_sems.at[2]).start()
    greeted(n)

    def line(source, target, stage):
        for i in range(1, groups):
            peer = lax.rem(plane + i, groups)
            send(
                source(peer),
                target.at[plane],
                send_sems.at[stage],
                recv_sems.at[stage],
                peer * members + place,
            )

    line(lambda peer: gated_ref, gated_buf, 2)
    loads[6].wait()
    drain(gated_buf, recv_sems.at[2])
    gated = gated_buf[...].reshape(gated_buf.shape[0] * gated_buf.shape[1], gated_buf.shape[2])
    mix_weight = weights[6][...]
    mix_weight = mix_weight.reshape(mix_weight.shape[0] * mix_weight.shape[1], mix_weight.shape[2])
    product_buf[...] = (
        lax.dot_general(
            gated, mix_weight, (((1,), (1,)), ((), ())), preferred_element_type=jnp.float32
        )
        .reshape(product_buf.shape)
        .astype(jnp.bfloat16)
    )
    pltpu.make_async_copy(product_buf.at[plane], mixed_buf.at[plane], recv_sems.at[3]).start()
    line(lambda peer: product_buf.at[peer], mixed_buf, 3)
    drain(mixed_buf, recv_sems.at[3])
    mixed = jnp.concatenate([mixed_buf[group] for group in range(groups)], axis=1)
    after_mix = (
        tokens_ref[...].astype(jnp.float32)
        + rms_scale(mixed.astype(jnp.float32), postmix_ref[...])
    ).astype(jnp.bfloat16)
    after_float = after_mix.astype(jnp.float32)
    token_rows = rms_scale(after_float, prefeed_ref[...]).astype(jnp.bfloat16)
    local, capacity = weights[0].shape[0], outgoing.shape[2]
    width = token_rows.shape[1]
    outgoing[...] = jnp.dot(
        dispatch_ref[...], token_rows, preferred_element_type=jnp.float32
    ).reshape(outgoing.shape).astype(jnp.bfloat16)
    pltpu.make_async_copy(outgoing.at[me], arrived.at[me], recv_sems.at[0]).start()

    def exchange(source, target, stage):
        def one(i, carry):
            peer = lax.rem(me + i, n)
            send(source.at[peer], target.at[me], send_sems.at[stage], recv_sems.at[stage], peer)
            return carry

        lax.fori_loop(1, n, one, 0)

    exchange(outgoing, arrived, 0)
    for index in (3, 4, 5):
        loads[index].wait()
    shared_out = two_layer(
        token_rows, weights[3][...], weights[4][...], weights[5][...]
    )
    for index in (0, 1, 2):
        loads[index].wait()
    drain(arrived, recv_sems.at[0])
    for item in range(local):
        block = arrived[:, item].astype(jnp.float32).reshape(n * capacity, width)
        answer[:, item] = (
            two_layer(
                block.astype(jnp.bfloat16),
                weights[0][item],
                weights[1][item],
                weights[2][item],
            )
            .reshape(n, capacity, width)
            .astype(jnp.bfloat16)
        )
    pltpu.make_async_copy(answer.at[me], returned.at[me], recv_sems.at[1]).start()
    exchange(answer, returned, 1)
    combine = combine_ref[...]
    high = combine.astype(jnp.bfloat16)
    low = (combine - high.astype(jnp.float32)).astype(jnp.bfloat16)
    drain(returned, recv_sems.at[1])
    picked = (
        returned[...].astype(jnp.float32).reshape(combine.shape[1], width).astype(jnp.bfloat16)
    )
    combined = (
        shared_out
        + jnp.dot(high, picked, preferred_element_type=jnp.float32)
        + jnp.dot(low, picked, preferred_element_type=jnp.float32)
    )
    out_ref[...] = (after_float + rms_scale(combined, postfeed_ref[...])).astype(jnp.bfloat16)
    drain(arrived.at[pl.ds(0, n - 1)], send_sems.at[0])
    drain(returned.at[pl.ds(0, n - 1)], send_sems.at[1])
    drain(gated_buf.at[pl.ds(0, groups - 1)], send_sems.at[2])
    drain(mixed_buf.at[pl.ds(0, groups - 1)], send_sems.at[3])


def tail(n, groups, gated, tokens, gains, dispatch, combine, *weights):
    sequences, width = tokens.shape
    local = weights[0].shape[0]
    capacity = dispatch.shape[0] // (n * local)
    slots = pltpu.VMEM((n, local, capacity, width), jnp.bfloat16)
    pieces = pltpu.VMEM((groups, sequences, width // groups), jnp.bfloat16)
    return pl.pallas_call(
        functools.partial(tail_kernel, n, groups),
        out_shape=jax.ShapeDtypeStruct((sequences, width), jnp.bfloat16),
        in_specs=[VM] * 7 + [ANY] * 7,
        out_specs=VM,
        scratch_shapes=[pltpu.VMEM(w.shape, w.dtype) for w in weights]
        + [pltpu.VMEM((groups,) + gated.shape, jnp.bfloat16), pieces, pieces]
        + [slots] * 4
        + [
            pltpu.SemaphoreType.DMA((7,)),
            pltpu.SemaphoreType.DMA((4,)),
            pltpu.SemaphoreType.DMA((4,)),
        ],
        compiler_params=pltpu.CompilerParams(
            collective_id=2, has_side_effects=True, vmem_limit_bytes=50 * 1024 * 1024
        ),
    )(gated, tokens, *(gain[None] for gain in gains), dispatch, combine, *weights)


def memory_step(
    queries,
    key_rows,
    value_rows,
    out_gate,
    input_pre,
    forget_pre,
    memory_state,
    normalizer,
    stabilizer,
):
    sequences = queries.shape[0]
    head_count = memory_state.shape[1]
    head_width = memory_state.shape[2]
    query_heads = queries.astype(jnp.float32).reshape(sequences, head_count, head_width)
    key_heads = key_rows.astype(jnp.float32).reshape(
        sequences, head_count, head_width
    ) * head_width ** (-0.5)
    value_heads = value_rows.astype(jnp.float32).reshape(sequences, head_count, head_width)
    carried = jax.nn.log_sigmoid(forget_pre) + stabilizer
    next_stabilizer = jnp.maximum(carried, input_pre)
    keep_old = jnp.exp(carried - next_stabilizer)
    write_new = jnp.exp(input_pre - next_stabilizer)
    local_score = write_new * jnp.sum(query_heads * key_heads, axis=-1)
    read_memory = jnp.einsum(
        "shvk,shk->shv", memory_state, query_heads, precision=lax.Precision.HIGHEST
    )
    numerator = keep_old[..., None] * read_memory + local_score[..., None] * value_heads
    denominator = keep_old * jnp.sum(normalizer * query_heads, axis=-1) + local_score
    memory_read = numerator / jnp.maximum(jnp.abs(denominator), 1.0)[..., None]
    gated_out = (
        jax.nn.sigmoid(out_gate.astype(jnp.float32))
        * memory_read.reshape(sequences, head_count * head_width)
    ).astype(jnp.bfloat16)
    next_memory = (
        keep_old[..., None, None] * memory_state
        + write_new[..., None, None] * value_heads[..., :, None] * key_heads[..., None, :]
    )
    next_normalizer = keep_old[..., None] * normalizer + write_new[..., None] * key_heads
    return (gated_out, next_memory, next_normalizer, next_stabilizer)


def on_device(
    tokens,
    premix_gain,
    postmix_gain,
    prefeed_gain,
    postfeed_gain,
    query_weight,
    key_weight,
    value_weight,
    outgate_weight,
    ingate_weight,
    forget_weight,
    ingate_bias,
    forget_bias,
    memory_state,
    normalizer,
    stabilizer,
    output_weight,
    expert_ids,
    route_weights,
    expert_gate,
    expert_up,
    expert_down,
    shared_gate,
    shared_up,
    shared_down,
):
    sequences = tokens.shape[0]
    model_width = tokens.shape[1]
    memory_width = query_weight.shape[1]
    devices = lax.axis_size("ep")
    residual = tokens.astype(jnp.float32)
    normed = rms_scale(residual, premix_gain).astype(jnp.bfloat16)
    projected, mix_weight = project(
        devices, GROUPS, normed, output_weight.T, query_weight, key_weight, value_weight, outgate_weight
    )
    projected = projected.reshape(sequences, 4, memory_width)
    input_pre = jnp.dot(normed, ingate_weight, preferred_element_type=jnp.float32) + ingate_bias
    forget_pre = jnp.dot(normed, forget_weight, preferred_element_type=jnp.float32) + forget_bias
    gated_out, next_memory, next_normalizer, next_stabilizer = memory_step(
        projected[:, 0],
        projected[:, 1],
        projected[:, 2],
        projected[:, 3],
        input_pre,
        forget_pre,
        memory_state,
        normalizer,
        stabilizer,
    )
    local_count = expert_gate.shape[0]
    experts_total = local_count * devices
    choose_count = expert_ids.shape[1]
    capacity = min(
        sequences, max(2, 2 * ((sequences * choose_count + experts_total - 1) // experts_total))
    )
    named = (expert_ids[:, :, None] == jnp.arange(experts_total, dtype=jnp.int32)).astype(
        jnp.float32
    )
    chosen = jnp.sum(named, axis=1)
    weight_of = jnp.sum(named * route_weights[:, :, None], axis=1)
    order = jnp.arange(sequences)
    before = (order[:, None] > order[None, :]).astype(jnp.float32)
    earlier = jnp.sum(before[:, :, None] * chosen[None, :, :], axis=1)
    slots = jnp.where(
        earlier[:, :, None] == jnp.arange(capacity, dtype=jnp.float32), chosen[:, :, None], 0.0
    )
    combine = (slots * weight_of[:, :, None]).reshape(sequences, experts_total * capacity)
    dispatch = slots.reshape(sequences, experts_total * capacity).T.astype(jnp.bfloat16)
    next_tokens = tail(
        devices,
        GROUPS,
        gated_out,
        tokens,
        (postmix_gain, prefeed_gain, postfeed_gain),
        dispatch,
        combine,
        expert_gate,
        expert_up,
        expert_down,
        shared_gate,
        shared_up,
        shared_down,
        mix_weight,
    )
    return (next_tokens, next_memory, next_normalizer, next_stabilizer)


def solution(mesh):
    in_specs = (
        P("ep", None),
        P(),
        P(),
        P(),
        P(),
        P("ep", None),
        P("ep", None),
        P("ep", None),
        P("ep", None),
        P(),
        P(),
        P(),
        P(),
        P("ep", None, None, None),
        P("ep", None, None),
        P("ep", None),
        P(None, "ep"),
        P("ep", None),
        P("ep", None),
        P("ep", None, None),
        P("ep", None, None),
        P("ep", None, None),
        P(),
        P(),
        P(),
    )
    out_specs = (P("ep", None), P("ep", None, None, None), P("ep", None, None), P("ep", None))
    return jax.shard_map(
        on_device, mesh=mesh, in_specs=in_specs, out_specs=out_specs, check_vma=False
    )
```

```python
import functools

import jax
import jax.numpy as jnp
from jax import lax
from jax.experimental import pallas as pl
from jax.experimental.pallas import tpu as pltpu
from jax.sharding import PartitionSpec as P

epsilon = 1e-06
LANES = 128
GROUPS = 4
MESH = pl.DeviceIdType.MESH
VM = pl.BlockSpec(memory_space=pltpu.VMEM)
ANY = pl.BlockSpec(memory_space=pl.ANY)


def rms_scale(values, gain_row):
    return (
        values * lax.rsqrt(jnp.mean(values * values, axis=-1, keepdims=True) + epsilon) * gain_row
    )


def greet(n, me):
    sem = pltpu.get_barrier_semaphore()

    def signal(i, carry):
        pl.semaphore_signal(
            sem, inc=1, device_id=(lax.rem(me + i, n),), device_id_type=MESH
        )
        return carry

    lax.fori_loop(1, n, signal, 0)


def greeted(n):
    pl.semaphore_wait(pltpu.get_barrier_semaphore(), n - 1)


def send(src, dst, send_sem, recv_sem, peer):
    pltpu.make_async_remote_copy(
        src_ref=src,
        dst_ref=dst,
        send_sem=send_sem,
        recv_sem=recv_sem,
        device_id=(peer,),
        device_id_type=MESH,
    ).start()


def drain(ref, sem):
    pltpu.make_async_copy(ref, ref, sem).wait()


def routing(ids, route_weights, slot_count, capacity):
    sequences, choices = ids.shape
    slot = lax.broadcasted_iota(jnp.int32, (sequences, slot_count), 1).astype(jnp.float32)
    owner = jnp.floor((slot + 0.5) * (1.0 / capacity))
    turn = slot - owner * capacity
    chosen = jnp.zeros((sequences, slot_count), jnp.float32)
    weight_of = jnp.zeros((sequences, slot_count), jnp.float32)
    float_ids = ids.astype(jnp.float32)
    for choice in range(choices):
        same = float_ids[:, choice : choice + 1] == owner
        chosen = jnp.where(same, 1.0, chosen)
        weight_of = jnp.where(same, route_weights[:, choice : choice + 1], weight_of)
    earlier = jnp.zeros((sequences, slot_count), jnp.float32)
    row = lax.broadcasted_iota(jnp.int32, (sequences, slot_count), 0)
    for other in range(sequences - 1):
        earlier = earlier + jnp.where(row > other, chosen[other : other + 1], 0.0)
    slots = jnp.where(earlier == turn, chosen, 0.0)
    return slots, slots * weight_of


def two_layer(rows, gate_weight, up_weight, down_weight):
    gate_values = jnp.dot(rows, gate_weight, preferred_element_type=jnp.float32)
    up_values = jnp.dot(rows, up_weight, preferred_element_type=jnp.float32)
    inner_rows = (gate_values * jax.nn.sigmoid(gate_values) * up_values).astype(jnp.bfloat16)
    return jnp.dot(inner_rows, down_weight, preferred_element_type=jnp.float32)


def layer_kernel(n, groups, *refs):
    (
        tokens_ref,
        premix_ref,
        postmix_ref,
        prefeed_ref,
        postfeed_ref,
        input_bias_ref,
        forget_bias_ref,
        normalizer_ref,
        stabilizer_ref,
        ids_ref,
        route_ref,
        mix_ref,
        query_ref,
        key_ref,
        value_ref,
        gate_ref,
    ) = refs[:16]
    loads_from = refs[16:25]
    out_ref, projected_ref, gates_ref = refs[25:28]
    loaded = refs[28:37]
    (
        normed_buf,
        rows_buf,
        weight_buf,
        product_buf,
        result_buf,
        mix_buf,
        split_buf,
        gated_src,
        gated_buf,
        columns_buf,
        mixed_buf,
        outgoing,
        arrived,
        answer,
        returned,
        load_sems,
        send_sems,
        recv_sems,
    ) = refs[37:]
    weights = loaded[:6]
    input_weight, forget_weight, memory = loaded[6:]
    me = lax.axis_index("ep")
    members = n // groups
    plane, place = me // members, lax.rem(me, members)
    part_width = rows_buf.shape[2]
    columns = weight_buf.shape[2]
    per_matrix = query_ref.shape[1] // columns
    greet(n, me)
    projections = (query_ref, key_ref, value_ref, gate_ref)

    def column(block):
        return pl.ds(pl.multiple_of(lax.rem(block, per_matrix) * columns, LANES), columns)

    for index, ref in enumerate(projections):

        @pl.when(place // per_matrix == index)
        def _():
            pltpu.make_async_copy(
                ref.at[:, column(place)], weight_buf.at[place], recv_sems.at[1]
            ).start()

    pltpu.make_async_copy(mix_ref, mix_buf.at[place], recv_sems.at[3]).start()
    loads = [
        pltpu.make_async_copy(source, target, load_sems.at[index])
        for index, (source, target) in enumerate(zip(loads_from, loaded))
    ]
    residual = tokens_ref[...].astype(jnp.float32)
    normed = rms_scale(residual, premix_ref[...]).astype(jnp.bfloat16)
    for group in range(groups):
        normed_buf[group] = normed[:, group * part_width : (group + 1) * part_width]
    pltpu.make_async_copy(normed_buf.at[plane], rows_buf.at[me], recv_sems.at[0]).start()
    greeted(n)

    def send_rows(i, carry):
        peer = lax.rem(me + i, n)
        send(
            normed_buf.at[peer // members],
            rows_buf.at[me],
            send_sems.at[0],
            recv_sems.at[0],
            peer,
        )
        return carry

    def send_weights(i, carry):
        block = lax.rem(place + i, members)
        for index, ref in enumerate(projections):

            @pl.when(block // per_matrix == index)
            def _():
                send(
                    ref.at[:, column(block)],
                    weight_buf.at[place],
                    send_sems.at[1],
                    recv_sems.at[1],
                    plane * members + block,
                )

        return carry

    lax.fori_loop(1, members, send_weights, 0)
    lax.fori_loop(1, n, send_rows, 0)
    for index in (6, 7, 8, 3, 4, 5, 0, 1, 2):
        loads[index].start()

    loads[6].wait()
    loads[7].wait()
    input_pre = (
        jnp.dot(normed, input_weight[...], preferred_element_type=jnp.float32)
        + input_bias_ref[...]
    )
    forget_pre = (
        jnp.dot(normed, forget_weight[...], preferred_element_type=jnp.float32)
        + forget_bias_ref[...]
    )
    carried = (
        jnp.minimum(forget_pre, 0.0)
        - jnp.log1p(jnp.exp(-jnp.abs(forget_pre)))
        + stabilizer_ref[...]
    )
    next_stabilizer = jnp.maximum(carried, input_pre)
    keep_old = jnp.exp(carried - next_stabilizer)
    write_new = jnp.exp(input_pre - next_stabilizer)
    gates_ref[0] = keep_old
    gates_ref[1] = write_new
    gates_ref[2] = next_stabilizer
    local, capacity, width = outgoing.shape[1:]
    slots, combine = routing(ids_ref[...], route_ref[...], n * local * capacity, capacity)
    dispatch = slots.T.astype(jnp.bfloat16)
    sequences, heads, head_width = memory.shape[:3]
    loads[8].wait()

    def split(s, carry):
        for head in range(heads):
            value = memory[s, head]
            high = value.astype(jnp.bfloat16)
            rows = pl.ds(pl.multiple_of(s * head_width, LANES), head_width)
            split_buf[head, rows, :head_width] = high
            split_buf[head, rows, head_width:] = (value - high.astype(jnp.float32)).astype(
                jnp.bfloat16
            )
        return carry

    lax.fori_loop(0, sequences, split, 0)

    drain(rows_buf, recv_sems.at[0])
    drain(weight_buf, recv_sems.at[1])
    rows = rows_buf[...].reshape(rows_buf.shape[0] * rows_buf.shape[1], part_width)
    weight = weight_buf[...].reshape(weight_buf.shape[0] * weight_buf.shape[1], columns)
    product = jnp.dot(rows, weight, preferred_element_type=jnp.float32)
    product_buf[...] = product.reshape(product_buf.shape).astype(jnp.bfloat16)
    pltpu.make_async_copy(product_buf.at[me], result_buf.at[me], recv_sems.at[2]).start()

    def exchange(source, target, stage):
        def one(i, carry):
            peer = lax.rem(me + i, n)
            send(source.at[peer], target.at[me], send_sems.at[stage], recv_sems.at[stage], peer)
            return carry

        lax.fori_loop(1, n, one, 0)

    def send_mix(i, carry):
        send(
            mix_ref,
            mix_buf.at[place],
            send_sems.at[3],
            recv_sems.at[3],
            plane * members + lax.rem(place + i, members),
        )
        return carry

    def line(source, target, stage):
        for i in range(1, groups):
            peer = lax.rem(plane + i, groups)
            send(
                source(peer),
                target.at[plane],
                send_sems.at[stage],
                recv_sems.at[stage],
                peer * members + place,
            )

    exchange(product_buf, result_buf, 2)
    lax.fori_loop(1, members, send_mix, 0)
    drain(result_buf, recv_sems.at[2])
    for member in range(members):
        total = result_buf[member].astype(jnp.float32)
        for group in range(1, groups):
            total = total + result_buf[group * members + member].astype(jnp.float32)
        total = total.astype(jnp.bfloat16).astype(jnp.float32)
        projected_ref[:, member * columns : (member + 1) * columns] = total
    memory_width = heads * head_width
    row = lax.broadcasted_iota(jnp.int32, (sequences, head_width), 0)
    for head in range(heads):

        def piece(matrix):
            start = matrix * memory_width + head * head_width
            return projected_ref[:, start : start + head_width]

        span = slice(head * head_width, (head + 1) * head_width)
        query, value, out_gate = piece(0), piece(2), piece(3)
        key = piece(1) * head_width ** (-0.5)
        keep, write = keep_old[:, head : head + 1], write_new[:, head : head + 1]
        local_score = write * jnp.sum(query * key, axis=-1, keepdims=True)
        denominator = (
            keep * jnp.sum(normalizer_ref[:, span] * query, axis=-1, keepdims=True) + local_score
        )
        narrow = query.astype(jnp.bfloat16)
        reads = lax.dot_general(
            jnp.concatenate([narrow, narrow], axis=1),
            split_buf[head],
            (((1,), (1,)), ((), ())),
            preferred_element_type=jnp.float32,
        )
        read = jnp.zeros((sequences, head_width), jnp.float32)
        for s in range(sequences):
            read = jnp.where(row == s, reads[:, s * head_width : (s + 1) * head_width], read)
        memory_read = (keep * read + local_score * value) / jnp.maximum(
            jnp.abs(denominator), 1.0
        )
        gated_src[:, span] = (jax.nn.sigmoid(out_gate) * memory_read).astype(jnp.bfloat16)

    pltpu.make_async_copy(gated_src, gated_buf.at[plane], recv_sems.at[4]).start()
    line(lambda peer: gated_src, gated_buf, 4)
    drain(mix_buf, recv_sems.at[3])
    drain(gated_buf, recv_sems.at[4])
    gated = gated_buf[...].reshape(gated_buf.shape[0] * gated_buf.shape[1], gated_buf.shape[2])
    mix_weight = mix_buf[...].reshape(mix_buf.shape[0] * mix_buf.shape[1], mix_buf.shape[2])
    columns_buf[...] = (
        lax.dot_general(
            gated, mix_weight, (((1,), (1,)), ((), ())), preferred_element_type=jnp.float32
        )
        .reshape(columns_buf.shape)
        .astype(jnp.bfloat16)
    )
    pltpu.make_async_copy(columns_buf.at[plane], mixed_buf.at[plane], recv_sems.at[5]).start()
    line(lambda peer: columns_buf.at[peer], mixed_buf, 5)
    drain(mixed_buf, recv_sems.at[5])
    mixed = jnp.concatenate([mixed_buf[group] for group in range(groups)], axis=1)
    after_mix = (residual + rms_scale(mixed.astype(jnp.float32), postmix_ref[...])).astype(
        jnp.bfloat16
    )
    after_float = after_mix.astype(jnp.float32)
    token_rows = rms_scale(after_float, prefeed_ref[...]).astype(jnp.bfloat16)
    outgoing[...] = (
        jnp.dot(dispatch, token_rows, preferred_element_type=jnp.float32)
        .reshape(outgoing.shape)
        .astype(jnp.bfloat16)
    )
    pltpu.make_async_copy(outgoing.at[me], arrived.at[me], recv_sems.at[6]).start()
    exchange(outgoing, arrived, 6)
    for index in (3, 4, 5):
        loads[index].wait()
    shared_out = two_layer(token_rows, weights[3][...], weights[4][...], weights[5][...])
    for index in (0, 1, 2):
        loads[index].wait()
    drain(arrived, recv_sems.at[6])
    for item in range(local):
        block = arrived[:, item].astype(jnp.float32).reshape(n * capacity, width)
        answer[:, item] = (
            two_layer(
                block.astype(jnp.bfloat16),
                weights[0][item],
                weights[1][item],
                weights[2][item],
            )
            .reshape(n, capacity, width)
            .astype(jnp.bfloat16)
        )
    pltpu.make_async_copy(answer.at[me], returned.at[me], recv_sems.at[7]).start()
    exchange(answer, returned, 7)
    high = combine.astype(jnp.bfloat16)
    low = (combine - high.astype(jnp.float32)).astype(jnp.bfloat16)
    drain(returned, recv_sems.at[7])
    picked = (
        returned[...].astype(jnp.float32).reshape(combine.shape[1], width).astype(jnp.bfloat16)
    )
    combined = (
        shared_out
        + jnp.dot(high, picked, preferred_element_type=jnp.float32)
        + jnp.dot(low, picked, preferred_element_type=jnp.float32)
    )
    out_ref[...] = (after_float + rms_scale(combined, postfeed_ref[...])).astype(jnp.bfloat16)
    drain(rows_buf.at[pl.ds(0, n - 1)], send_sems.at[0])
    drain(weight_buf.at[pl.ds(0, members - 1)], send_sems.at[1])
    drain(result_buf.at[pl.ds(0, n - 1)], send_sems.at[2])
    drain(mix_buf.at[pl.ds(0, members - 1)], send_sems.at[3])
    drain(gated_buf.at[pl.ds(0, groups - 1)], send_sems.at[4])
    drain(mixed_buf.at[pl.ds(0, groups - 1)], send_sems.at[5])
    drain(arrived.at[pl.ds(0, n - 1)], send_sems.at[6])
    drain(returned.at[pl.ds(0, n - 1)], send_sems.at[7])


def layer(n, groups, small, projections, loads, capacity):
    tokens, mix_weight = small[0], small[-1]
    sequences, width = tokens.shape
    depth, columns = projections[0].shape
    members = n // groups
    wide = 4 * columns // members
    local = loads[0].shape[0]
    heads, head_width = loads[8].shape[1:3]
    narrow = functools.partial(pltpu.VMEM, dtype=jnp.bfloat16)
    slots = narrow((n, local, capacity, width))
    pieces = narrow((groups, sequences, width // groups))
    return pl.pallas_call(
        functools.partial(layer_kernel, n, groups),
        out_shape=(
            jax.ShapeDtypeStruct((sequences, width), jnp.bfloat16),
            jax.ShapeDtypeStruct((sequences, 4 * columns), jnp.float32),
            jax.ShapeDtypeStruct((3, sequences, heads), jnp.float32),
        ),
        in_specs=[VM] * len(small) + [ANY] * (len(projections) + len(loads)),
        out_specs=(VM, VM, VM),
        scratch_shapes=[pltpu.VMEM(w.shape, w.dtype) for w in loads]
        + [
            pieces,
            narrow((n, sequences, width // groups)),
            narrow((members, depth, wide)),
            narrow((n, sequences, wide)),
            narrow((n, sequences, wide)),
            narrow((members,) + mix_weight.shape),
            narrow((heads, sequences * head_width, 2 * head_width)),
            narrow((sequences, columns)),
            narrow((groups, sequences, columns)),
            pieces,
            pieces,
        ]
        + [slots] * 4
        + [
            pltpu.SemaphoreType.DMA((len(loads),)),
            pltpu.SemaphoreType.DMA((8,)),
            pltpu.SemaphoreType.DMA((8,)),
        ],
        compiler_params=pltpu.CompilerParams(
            collective_id=0, has_side_effects=True, vmem_limit_bytes=56 * 1024 * 1024
        ),
    )(*small, *projections, *loads)


def on_device(
    tokens,
    premix_gain,
    postmix_gain,
    prefeed_gain,
    postfeed_gain,
    query_weight,
    key_weight,
    value_weight,
    outgate_weight,
    ingate_weight,
    forget_weight,
    ingate_bias,
    forget_bias,
    memory_state,
    normalizer,
    stabilizer,
    output_weight,
    expert_ids,
    route_weights,
    expert_gate,
    expert_up,
    expert_down,
    shared_gate,
    shared_up,
    shared_down,
):
    sequences = tokens.shape[0]
    memory_width = query_weight.shape[1]
    heads, head_width = memory_state.shape[1:3]
    devices = lax.axis_size("ep")
    experts_total = expert_gate.shape[0] * devices
    choose_count = expert_ids.shape[1]
    capacity = min(
        sequences, max(2, 2 * ((sequences * choose_count + experts_total - 1) // experts_total))
    )
    next_tokens, projected, gates = layer(
        devices,
        GROUPS,
        (
            tokens,
            premix_gain[None],
            postmix_gain[None],
            prefeed_gain[None],
            postfeed_gain[None],
            ingate_bias[None],
            forget_bias[None],
            normalizer.reshape(sequences, memory_width),
            stabilizer,
            expert_ids,
            route_weights,
            output_weight.T,
        ),
        (query_weight, key_weight, value_weight, outgate_weight),
        (
            expert_gate,
            expert_up,
            expert_down,
            shared_gate,
            shared_up,
            shared_down,
            ingate_weight,
            forget_weight,
            memory_state,
        ),
        capacity,
    )
    keep_old, write_new, next_stabilizer = gates[0], gates[1], gates[2]
    split = projected.reshape(sequences, 4, heads, head_width)
    key_heads = split[:, 1] * head_width ** (-0.5)
    value_heads = split[:, 2]
    next_memory = (
        keep_old[..., None, None] * memory_state
        + write_new[..., None, None] * value_heads[..., :, None] * key_heads[..., None, :]
    )
    next_normalizer = keep_old[..., None] * normalizer + write_new[..., None] * key_heads
    return (next_tokens, next_memory, next_normalizer, next_stabilizer)


def solution(mesh):
    in_specs = (
        P("ep", None),
        P(),
        P(),
        P(),
        P(),
        P("ep", None),
        P("ep", None),
        P("ep", None),
        P("ep", None),
        P(),
        P(),
        P(),
        P(),
        P("ep", None, None, None),
        P("ep", None, None),
        P("ep", None),
        P(None, "ep"),
        P("ep", None),
        P("ep", None),
        P("ep", None, None),
        P("ep", None, None),
        P("ep", None, None),
        P(),
        P(),
        P(),
    )
    out_specs = (P("ep", None), P("ep", None, None, None), P("ep", None, None), P("ep", None))
    return jax.shard_map(
        on_device, mesh=mesh, in_specs=in_specs, out_specs=out_specs, check_vma=False
    )
```

```python
import functools

import jax
import jax.numpy as jnp
from jax import lax
from jax.experimental import pallas as pl
from jax.experimental.pallas import tpu as pltpu
from jax.sharding import PartitionSpec as P

epsilon = 1e-06
LANES = 128
GROUPS = 4
MESH = pl.DeviceIdType.MESH
VM = pl.BlockSpec(memory_space=pltpu.VMEM)
ANY = pl.BlockSpec(memory_space=pl.ANY)


def rms_scale(values, gain_row):
    return (
        values * lax.rsqrt(jnp.mean(values * values, axis=-1, keepdims=True) + epsilon) * gain_row
    )


def greet(n, me):
    sem = pltpu.get_barrier_semaphore()

    def signal(i, carry):
        pl.semaphore_signal(
            sem, inc=1, device_id=(lax.rem(me + i, n),), device_id_type=MESH
        )
        return carry

    lax.fori_loop(1, n, signal, 0)


def greeted(n):
    pl.semaphore_wait(pltpu.get_barrier_semaphore(), n - 1)


def send(src, dst, send_sem, recv_sem, peer):
    pltpu.make_async_remote_copy(
        src_ref=src,
        dst_ref=dst,
        send_sem=send_sem,
        recv_sem=recv_sem,
        device_id=(peer,),
        device_id_type=MESH,
    ).start()


def drain(ref, sem):
    pltpu.make_async_copy(ref, ref, sem).wait()


def routing(ids, route_weights, slot_count, capacity):
    sequences, choices = ids.shape
    slot = lax.broadcasted_iota(jnp.int32, (sequences, slot_count), 1).astype(jnp.float32)
    owner = jnp.floor((slot + 0.5) * (1.0 / capacity))
    turn = slot - owner * capacity
    chosen = jnp.zeros((sequences, slot_count), jnp.float32)
    weight_of = jnp.zeros((sequences, slot_count), jnp.float32)
    float_ids = ids.astype(jnp.float32)
    for choice in range(choices):
        same = float_ids[:, choice : choice + 1] == owner
        chosen = jnp.where(same, 1.0, chosen)
        weight_of = jnp.where(same, route_weights[:, choice : choice + 1], weight_of)
    earlier = jnp.zeros((sequences, slot_count), jnp.float32)
    row = lax.broadcasted_iota(jnp.int32, (sequences, slot_count), 0)
    for other in range(sequences - 1):
        earlier = earlier + jnp.where(row > other, chosen[other : other + 1], 0.0)
    slots = jnp.where(earlier == turn, chosen, 0.0)
    return slots, slots * weight_of


def across(left, right):
    return lax.dot_general(
        left, right, (((1,), (1,)), ((), ())), preferred_element_type=jnp.float32
    )


def two_layer(rows, gate_weight, up_weight, down_weight):
    gate_values = jnp.dot(rows, gate_weight, preferred_element_type=jnp.float32)
    up_values = jnp.dot(rows, up_weight, preferred_element_type=jnp.float32)
    inner_rows = (gate_values * jax.nn.sigmoid(gate_values) * up_values).astype(jnp.bfloat16)
    return jnp.dot(inner_rows, down_weight, preferred_element_type=jnp.float32)


def layer_kernel(n, groups, *refs):
    (
        tokens_ref,
        premix_ref,
        postmix_ref,
        prefeed_ref,
        postfeed_ref,
        input_bias_ref,
        forget_bias_ref,
        normalizer_ref,
        stabilizer_ref,
        ids_ref,
        route_ref,
        mix_ref,
        query_ref,
        key_ref,
        value_ref,
        gate_ref,
    ) = refs[:16]
    loads_from = refs[16:25]
    out_ref, projected_ref, gates_ref = refs[25:28]
    loaded = refs[28:37]
    (
        normed_buf,
        rows_buf,
        weight_buf,
        product_buf,
        result_buf,
        mix_buf,
        split_buf,
        gated_src,
        gated_buf,
        columns_buf,
        mixed_buf,
        outgoing,
        arrived,
        answer,
        returned,
        load_sems,
        send_sems,
        recv_sems,
    ) = refs[37:]
    weights = loaded[:6]
    input_weight, forget_weight, memory = loaded[6:]
    me = lax.axis_index("ep")
    members = n // groups
    plane, place = me // members, lax.rem(me, members)
    part_width = rows_buf.shape[2]
    columns = weight_buf.shape[2]
    per_matrix = query_ref.shape[1] // columns
    greet(n, me)
    projections = (query_ref, key_ref, value_ref, gate_ref)

    def column(block):
        return pl.ds(pl.multiple_of(lax.rem(block, per_matrix) * columns, LANES), columns)

    for index, ref in enumerate(projections):

        @pl.when(place // per_matrix == index)
        def _():
            pltpu.make_async_copy(
                ref.at[:, column(place)], weight_buf.at[place], recv_sems.at[1]
            ).start()

    pltpu.make_async_copy(mix_ref, mix_buf.at[place], recv_sems.at[3]).start()
    loads = [
        pltpu.make_async_copy(source, target, load_sems.at[index])
        for index, (source, target) in enumerate(zip(loads_from, loaded))
    ]
    residual = tokens_ref[...].astype(jnp.float32)
    normed = rms_scale(residual, premix_ref[...]).astype(jnp.bfloat16)
    for group in range(groups):
        normed_buf[group] = normed[:, group * part_width : (group + 1) * part_width]
    pltpu.make_async_copy(normed_buf.at[plane], rows_buf.at[me], recv_sems.at[0]).start()
    greeted(n)

    def send_rows(i, carry):
        peer = lax.rem(me + i, n)
        send(
            normed_buf.at[peer // members],
            rows_buf.at[me],
            send_sems.at[0],
            recv_sems.at[0],
            peer,
        )
        return carry

    def send_weights(i, carry):
        block = lax.rem(place + i, members)
        for index, ref in enumerate(projections):

            @pl.when(block // per_matrix == index)
            def _():
                send(
                    ref.at[:, column(block)],
                    weight_buf.at[place],
                    send_sems.at[1],
                    recv_sems.at[1],
                    plane * members + block,
                )

        return carry

    lax.fori_loop(1, members, send_weights, 0)
    lax.fori_loop(1, n, send_rows, 0)
    for index in (6, 7, 8, 3, 4, 5, 0, 1, 2):
        loads[index].start()

    loads[6].wait()
    loads[7].wait()
    input_pre = (
        across(normed, input_weight[...])
        + input_bias_ref[...]
    )
    forget_pre = (
        across(normed, forget_weight[...])
        + forget_bias_ref[...]
    )
    carried = (
        jnp.minimum(forget_pre, 0.0)
        - jnp.log1p(jnp.exp(-jnp.abs(forget_pre)))
        + stabilizer_ref[...]
    )
    next_stabilizer = jnp.maximum(carried, input_pre)
    keep_old = jnp.exp(carried - next_stabilizer)
    write_new = jnp.exp(input_pre - next_stabilizer)
    gates_ref[0] = keep_old
    gates_ref[1] = write_new
    gates_ref[2] = next_stabilizer
    local, capacity, width = outgoing.shape[1:]
    slots, combine = routing(ids_ref[...], route_ref[...], n * local * capacity, capacity)
    dispatch = slots.T.astype(jnp.bfloat16)
    sequences, heads, head_width = memory.shape[:3]
    loads[8].wait()

    def split(s, carry):
        for head in range(heads):
            value = memory[s, head]
            high = value.astype(jnp.bfloat16)
            rows = pl.ds(pl.multiple_of(s * head_width, LANES), head_width)
            split_buf[head, rows, :head_width] = high
            split_buf[head, rows, head_width:] = (value - high.astype(jnp.float32)).astype(
                jnp.bfloat16
            )
        return carry

    lax.fori_loop(0, sequences, split, 0)

    drain(rows_buf, recv_sems.at[0])
    drain(weight_buf, recv_sems.at[1])
    rows = rows_buf[...].reshape(rows_buf.shape[0] * rows_buf.shape[1], part_width)
    weight = weight_buf[...].reshape(weight_buf.shape[0] * weight_buf.shape[1], columns)
    product = jnp.dot(rows, weight, preferred_element_type=jnp.float32)
    product_buf[...] = product.reshape(product_buf.shape).astype(jnp.bfloat16)
    pltpu.make_async_copy(product_buf.at[me], result_buf.at[me], recv_sems.at[2]).start()

    def exchange(source, target, stage):
        def one(i, carry):
            peer = lax.rem(me + i, n)
            send(source.at[peer], target.at[me], send_sems.at[stage], recv_sems.at[stage], peer)
            return carry

        lax.fori_loop(1, n, one, 0)

    def send_mix(i, carry):
        send(
            mix_ref,
            mix_buf.at[place],
            send_sems.at[3],
            recv_sems.at[3],
            plane * members + lax.rem(place + i, members),
        )
        return carry

    def line(source, target, stage):
        for i in range(1, groups):
            peer = lax.rem(plane + i, groups)
            send(
                source(peer),
                target.at[plane],
                send_sems.at[stage],
                recv_sems.at[stage],
                peer * members + place,
            )

    exchange(product_buf, result_buf, 2)
    lax.fori_loop(1, members, send_mix, 0)
    drain(result_buf, recv_sems.at[2])
    for member in range(members):
        total = result_buf[member].astype(jnp.float32)
        for group in range(1, groups):
            total = total + result_buf[group * members + member].astype(jnp.float32)
        total = total.astype(jnp.bfloat16).astype(jnp.float32)
        projected_ref[:, member * columns : (member + 1) * columns] = total
    memory_width = heads * head_width
    row = lax.broadcasted_iota(jnp.int32, (sequences, head_width), 0)
    for head in range(heads):

        def piece(matrix):
            start = matrix * memory_width + head * head_width
            return projected_ref[:, start : start + head_width]

        span = slice(head * head_width, (head + 1) * head_width)
        query, value, out_gate = piece(0), piece(2), piece(3)
        key = piece(1) * head_width ** (-0.5)
        keep, write = keep_old[:, head : head + 1], write_new[:, head : head + 1]
        local_score = write * jnp.sum(query * key, axis=-1, keepdims=True)
        denominator = (
            keep * jnp.sum(normalizer_ref[:, head, :] * query, axis=-1, keepdims=True) + local_score
        )
        narrow = query.astype(jnp.bfloat16)
        reads = lax.dot_general(
            jnp.concatenate([narrow, narrow], axis=1),
            split_buf[head],
            (((1,), (1,)), ((), ())),
            preferred_element_type=jnp.float32,
        )
        read = jnp.zeros((sequences, head_width), jnp.float32)
        for s in range(sequences):
            read = jnp.where(row == s, reads[:, s * head_width : (s + 1) * head_width], read)
        memory_read = (keep * read + local_score * value) / jnp.maximum(
            jnp.abs(denominator), 1.0
        )
        gated_src[:, span] = (jax.nn.sigmoid(out_gate) * memory_read).astype(jnp.bfloat16)

    pltpu.make_async_copy(gated_src, gated_buf.at[plane], recv_sems.at[4]).start()
    line(lambda peer: gated_src, gated_buf, 4)
    drain(mix_buf, recv_sems.at[3])
    drain(gated_buf, recv_sems.at[4])
    gated = gated_buf[...].reshape(gated_buf.shape[0] * gated_buf.shape[1], gated_buf.shape[2])
    mix_weight = mix_buf[...].reshape(mix_buf.shape[0] * mix_buf.shape[1], mix_buf.shape[2])
    columns_buf[...] = (
        lax.dot_general(
            gated, mix_weight, (((1,), (1,)), ((), ())), preferred_element_type=jnp.float32
        )
        .reshape(columns_buf.shape)
        .astype(jnp.bfloat16)
    )
    pltpu.make_async_copy(columns_buf.at[plane], mixed_buf.at[plane], recv_sems.at[5]).start()
    line(lambda peer: columns_buf.at[peer], mixed_buf, 5)
    drain(mixed_buf, recv_sems.at[5])
    mixed = jnp.concatenate([mixed_buf[group] for group in range(groups)], axis=1)
    after_mix = (residual + rms_scale(mixed.astype(jnp.float32), postmix_ref[...])).astype(
        jnp.bfloat16
    )
    after_float = after_mix.astype(jnp.float32)
    token_rows = rms_scale(after_float, prefeed_ref[...]).astype(jnp.bfloat16)
    outgoing[...] = (
        jnp.dot(dispatch, token_rows, preferred_element_type=jnp.float32)
        .reshape(outgoing.shape)
        .astype(jnp.bfloat16)
    )
    pltpu.make_async_copy(outgoing.at[me], arrived.at[me], recv_sems.at[6]).start()
    exchange(outgoing, arrived, 6)
    for index in (3, 4, 5):
        loads[index].wait()
    shared_out = two_layer(token_rows, weights[3][...], weights[4][...], weights[5][...])
    for index in (0, 1, 2):
        loads[index].wait()
    drain(arrived, recv_sems.at[6])
    for item in range(local):
        block = arrived[:, item].astype(jnp.float32).reshape(n * capacity, width)
        answer[:, item] = (
            two_layer(
                block.astype(jnp.bfloat16),
                weights[0][item],
                weights[1][item],
                weights[2][item],
            )
            .reshape(n, capacity, width)
            .astype(jnp.bfloat16)
        )
    pltpu.make_async_copy(answer.at[me], returned.at[me], recv_sems.at[7]).start()
    exchange(answer, returned, 7)
    high = combine.astype(jnp.bfloat16)
    low = (combine - high.astype(jnp.float32)).astype(jnp.bfloat16)
    drain(returned, recv_sems.at[7])
    picked = (
        returned[...].astype(jnp.float32).reshape(combine.shape[1], width).astype(jnp.bfloat16)
    )
    combined = (
        shared_out
        + jnp.dot(high, picked, preferred_element_type=jnp.float32)
        + jnp.dot(low, picked, preferred_element_type=jnp.float32)
    )
    out_ref[...] = (after_float + rms_scale(combined, postfeed_ref[...])).astype(jnp.bfloat16)
    drain(rows_buf.at[pl.ds(0, n - 1)], send_sems.at[0])
    drain(weight_buf.at[pl.ds(0, members - 1)], send_sems.at[1])
    drain(result_buf.at[pl.ds(0, n - 1)], send_sems.at[2])
    drain(mix_buf.at[pl.ds(0, members - 1)], send_sems.at[3])
    drain(gated_buf.at[pl.ds(0, groups - 1)], send_sems.at[4])
    drain(mixed_buf.at[pl.ds(0, groups - 1)], send_sems.at[5])
    drain(arrived.at[pl.ds(0, n - 1)], send_sems.at[6])
    drain(returned.at[pl.ds(0, n - 1)], send_sems.at[7])


def layer(n, groups, small, projections, loads, capacity):
    tokens, mix_weight = small[0], small[-1]
    sequences, width = tokens.shape
    depth, columns = projections[0].shape
    members = n // groups
    wide = 4 * columns // members
    local = loads[0].shape[0]
    heads, head_width = loads[8].shape[1:3]
    narrow = functools.partial(pltpu.VMEM, dtype=jnp.bfloat16)
    slots = narrow((n, local, capacity, width))
    pieces = narrow((groups, sequences, width // groups))
    return pl.pallas_call(
        functools.partial(layer_kernel, n, groups),
        out_shape=(
            jax.ShapeDtypeStruct((sequences, width), jnp.bfloat16),
            jax.ShapeDtypeStruct((sequences, 4 * columns), jnp.float32),
            jax.ShapeDtypeStruct((3, sequences, heads), jnp.float32),
        ),
        in_specs=[VM] * len(small) + [ANY] * (len(projections) + len(loads)),
        out_specs=(VM, VM, VM),
        scratch_shapes=[pltpu.VMEM(w.shape, w.dtype) for w in loads]
        + [
            pieces,
            narrow((n, sequences, width // groups)),
            narrow((members, depth, wide)),
            narrow((n, sequences, wide)),
            narrow((n, sequences, wide)),
            narrow((members,) + mix_weight.shape),
            narrow((heads, sequences * head_width, 2 * head_width)),
            narrow((sequences, columns)),
            narrow((groups, sequences, columns)),
            pieces,
            pieces,
        ]
        + [slots] * 4
        + [
            pltpu.SemaphoreType.DMA((len(loads),)),
            pltpu.SemaphoreType.DMA((8,)),
            pltpu.SemaphoreType.DMA((8,)),
        ],
        compiler_params=pltpu.CompilerParams(
            collective_id=0, has_side_effects=True, vmem_limit_bytes=56 * 1024 * 1024
        ),
    )(*small, *projections, *loads)


def state_kernel(
    tokens_ref,
    projected_ref,
    gates_ref,
    normalizer_ref,
    memory_ref,
    next_tokens_ref,
    next_memory_ref,
    next_normalizer_ref,
    next_stabilizer_ref,
):
    step = pl.program_id(0)
    block, heads, head_width = memory_ref.shape[:3]
    memory_width = heads * head_width
    scale = head_width ** (-0.5)

    @pl.when(step == 0)
    def _():
        next_tokens_ref[...] = tokens_ref[...]
        next_stabilizer_ref[...] = gates_ref[2]
        keep_all, write_all = gates_ref[0], gates_ref[1]
        for head in range(heads):
            start = memory_width + head * head_width
            next_normalizer_ref[:, head, :] = keep_all[:, head : head + 1] * normalizer_ref[
                :, head, :
            ] + write_all[:, head : head + 1] * (
                projected_ref[:, start : start + head_width] * scale
            )

    for item in range(block):
        row = pl.ds(step * block + item, 1)
        keep, write = gates_ref[0, row, :], gates_ref[1, row, :]
        keys = projected_ref[row, memory_width : 2 * memory_width] * scale
        values = projected_ref[row, 2 * memory_width : 3 * memory_width]
        stacked = jnp.concatenate(
            [
                write[:, head : head + 1] * values[:, head * head_width : (head + 1) * head_width]
                for head in range(heads)
            ],
            axis=0,
        ).T
        for head in range(heads):
            next_memory_ref[item, head] = (
                keep[:, head : head + 1] * memory_ref[item, head]
                + stacked[:, head : head + 1]
                * keys[:, head * head_width : (head + 1) * head_width]
            )


def write_state(tokens, projected, gates, normalizer, memory):
    sequences = memory.shape[0]
    steps = 4
    block = (sequences // steps,) + memory.shape[1:]

    def whole(array):
        return pl.BlockSpec(array.shape, lambda i, rank=array.ndim: (0,) * rank)

    moving = pl.BlockSpec(block, lambda i: (i, 0, 0, 0))
    stabilizer = jax.ShapeDtypeStruct(gates.shape[1:], jnp.float32)
    return pl.pallas_call(
        state_kernel,
        grid=(steps,),
        out_shape=(
            jax.ShapeDtypeStruct(tokens.shape, tokens.dtype),
            jax.ShapeDtypeStruct(memory.shape, memory.dtype),
            jax.ShapeDtypeStruct(normalizer.shape, normalizer.dtype),
            stabilizer,
        ),
        in_specs=[whole(tokens), whole(projected), whole(gates), whole(normalizer), moving],
        out_specs=(whole(tokens), moving, whole(normalizer), whole(stabilizer)),
        compiler_params=pltpu.CompilerParams(dimension_semantics=("arbitrary",)),
    )(tokens, projected, gates, normalizer, memory)


def on_device(
    tokens,
    premix_gain,
    postmix_gain,
    prefeed_gain,
    postfeed_gain,
    query_weight,
    key_weight,
    value_weight,
    outgate_weight,
    ingate_weight,
    forget_weight,
    ingate_bias,
    forget_bias,
    memory_state,
    normalizer,
    stabilizer,
    output_weight,
    expert_ids,
    route_weights,
    expert_gate,
    expert_up,
    expert_down,
    shared_gate,
    shared_up,
    shared_down,
):
    sequences = tokens.shape[0]
    devices = lax.axis_size("ep")
    experts_total = expert_gate.shape[0] * devices
    choose_count = expert_ids.shape[1]
    capacity = min(
        sequences, max(2, 2 * ((sequences * choose_count + experts_total - 1) // experts_total))
    )
    next_tokens, projected, gates = layer(
        devices,
        GROUPS,
        (
            tokens,
            premix_gain[None],
            postmix_gain[None],
            prefeed_gain[None],
            postfeed_gain[None],
            ingate_bias[None],
            forget_bias[None],
            normalizer,
            stabilizer,
            expert_ids,
            route_weights,
            output_weight.T,
        ),
        (query_weight, key_weight, value_weight, outgate_weight),
        (
            expert_gate,
            expert_up,
            expert_down,
            shared_gate,
            shared_up,
            shared_down,
            ingate_weight.T,
            forget_weight.T,
            memory_state,
        ),
        capacity,
    )
    return write_state(next_tokens, projected, gates, normalizer, memory_state)


def solution(mesh):
    in_specs = (
        P("ep", None),
        P(),
        P(),
        P(),
        P(),
        P("ep", None),
        P("ep", None),
        P("ep", None),
        P("ep", None),
        P(),
        P(),
        P(),
        P(),
        P("ep", None, None, None),
        P("ep", None, None),
        P("ep", None),
        P(None, "ep"),
        P("ep", None),
        P("ep", None),
        P("ep", None, None),
        P("ep", None, None),
        P("ep", None, None),
        P(),
        P(),
        P(),
    )
    out_specs = (P("ep", None), P("ep", None, None, None), P("ep", None, None), P("ep", None))
    return jax.shard_map(
        on_device, mesh=mesh, in_specs=in_specs, out_specs=out_specs, check_vma=False
    )
```
